32 devices in a mesh: grp: 2 (over x), sp: 4 (over y, core), tp: 4 (over z).
Axes of the slice: x: 2, y: 2, z: 4, core: 2. Of those that a mesh axis runs over, the one named last changes fastest.
Arguments:
- residual: bfloat16 [768, 8, 2048], P(('sp', 'tp'), 'grp'), parts along dimension 1, may hold values from -6 to 6
- query: bfloat16 [768, 8, 1536], P('sp', 'grp', 'tp'), parts along dimension 1, may hold values from -64 to 64
- latent: bfloat16 [768, 8, 512], P('sp', 'grp'), parts along dimension 1, may hold values from -6 to 6
- rope_key: bfloat16 [768, 8, 64], P('sp', 'grp'), parts along dimension 1, may hold values from -8 to 8
- latent_gain: float32 [512], replicated, may hold values from 0.1 to 1.9
- key_up: bfloat16 [512, 1024], P(None, 'tp'), may hold values from -0.25 to 0.25
- value_up: bfloat16 [512, 1024], P(None, 'tp'), may hold values from -0.25 to 0.25
- out_weight: bfloat16 [1024, 2048], P('tp'), may hold values from -0.375 to 0.375
- norm_gain: float32 [2048], replicated, may hold values from 0.1 to 1.9
- group_prob: float32 [768, 8], P(('sp', 'tp'), 'grp'), parts along dimension 1, may hold values from 0.25 to 1
- pair_logits: float32 [768, 8, 2], P(('sp', 'tp'), 'grp'), parts along dimension 1, may hold values from -8 to 8
- routes: int32 [768, 8, 2], P(('sp', 'tp'), 'grp'), parts along dimension 1, may hold values from 0 to 15, all different within a row; in each aligned block of 192 rows (0 to 191, 192 to 383, ..., all dimensions but the last counted through in order) at most 36 rows name the same one
- w_gate: bfloat16 [16, 2048, 768], P(('sp', 'tp')), may hold values from -0.125 to 0.125
- w_up: bfloat16 [16, 2048, 768], P(('sp', 'tp')), may hold values from -0.125 to 0.125
- w_down: bfloat16 [16, 768, 2048], P(('sp', 'tp')), may hold values from -0.4375 to 0.4375
Outputs:
- layer_out: bfloat16 [768, 8, 2048], P(('sp', 'tp'), 'grp'), parts along dimension 1
The draws below stay inside these ranges and needn't reach their ends.
There are 2 independent parts, one for each index of `grp`. The reference program is written for one: setup_inputs(seed, part) draws one part's arguments, and reference() takes and returns one part's arrays. A program takes and returns all parts, laid end to end along the dimension named above; an argument that names none is the same for every part. Nothing has to cross between parts.
Inputs may be any that keep to these rules, and one draw needn't show every extreme that they name: `routes`: A token's 2 experts differ. Among the tokens of one device (aligned blocks of 192 rows in position-then-sequence order), no expert is named more than 36 times, a bound that some block reaches.
All inputs are finite; a program needn't handle non-finite values.
Results may differ from the reference program's by a relative error of at most 0.013.
Values may be sent and summed in bfloat16 or wider, within the bound.
A program may use at most 128 MiB of HBM per device.

```python
import math
import jax
import jax.numpy as jnp
import numpy as np
from jax import lax

D = 2048
HEADS = 8
NOPE = 128
ROPE = 64
VDIM = 128
QK = 192
LATENT = 512
FF = 768
TOPK = 2
SEQS = 4
LEN = 768
ROWS_DEV = 192
EXPERTS = 16
CAP = 36


def draw_rope_key(key, part):
    shape_all = (LEN, SEQS, ROPE)
    drawn = jnp.clip(jax.random.normal(jax.random.fold_in(key, 2), shape_all, jnp.float32), -6.0, 6.0)
    return drawn.astype(jnp.bfloat16)


def draw_query(key, part):
    shape_all = (LEN, SEQS, HEADS * QK)
    drawn = jnp.clip(2.5 * jax.random.normal(jax.random.fold_in(key, 1), shape_all, jnp.float32), -15.0, 15.0)
    return drawn.astype(jnp.bfloat16)


def block_levels(rng, dims, pieces, least, top_value):
    gain, own = 1.0, jax.random.fold_in(rng, 6)
    for position, blocks in pieces:
        steps = jnp.exp(jax.random.uniform(jax.random.fold_in(own, position), (blocks,), jnp.float32, least / len(pieces), top_value / len(pieces)))
        gain = gain * jnp.repeat(steps, dims[position] // blocks).reshape([-1 if axis == position else 1 for axis in range(len(dims))])
    return gain


def assign_block(stream_key, own, number, rows, count, top, bound, skew):
    order = jax.random.permutation(stream_key, count)
    packed, common = load_shares(count, rows * top, bound, skew, True), load_shares(count, rows * top, bound, skew, False)
    places = jnp.arange(count)

    def named(lengths, rotation):
        used = int((lengths > 0).sum())
        fixed = max(1, used // 4)
        moved = fixed + (places - fixed + rotation * (used - fixed)) % max(1, count - fixed)
        return jnp.zeros((count,), jnp.int32).at[order[jnp.where(places < fixed, places, moved)]].set(jnp.asarray(lengths, jnp.int32))

    lengths = jnp.where(number % 4 == 0, named(packed, number // 4), named(common, number - number // 4 - 1))
    mixed = jax.random.permutation(jax.random.fold_in(own, 3), count)
    giver, taker = mixed[0:count // 2 * 2:2], mixed[1:count // 2 * 2:2]
    slack = jnp.minimum(lengths[giver] - 1, bound - lengths[taker]) // 2
    slack = jnp.where((giver == order[0]) | (taker == order[0]) | (lengths[taker] == 0), 0, jnp.maximum(slack, 0))
    moved = jax.random.randint(jax.random.fold_in(own, 4), (count // 2,), 0, 1 << 20) % (slack + 1)
    lengths = lengths.at[giver].add(-moved).at[taker].add(moved)
    members = jnp.searchsorted(jnp.cumsum(lengths), jnp.arange(rows * top), side="right").astype(jnp.int32)
    listing = members.reshape(top, rows).T
    listing = listing[jax.random.permutation(jax.random.fold_in(own, 1), rows)]
    rotation = jax.random.randint(jax.random.fold_in(own, 2), (rows, 1), 0, top)
    return jnp.take_along_axis(listing, (jnp.arange(top)[None, :] + rotation) % top, axis=1)


def load_shares(count, total, reach, slope, full):
    portions = [(1 << 20) // math.isqrt(grade ** slope) + 1 for grade in range(1, count + 1)]
    largest = reach if full else min(reach, max(-(-total // count), total * portions[0] // sum(portions)))
    least = 1 if total - largest >= count - 1 else 0
    given, rest = [largest] + [least] * (count - 1), total - largest - least * (count - 1)
    while rest > 0:
        free = [i for i in range(1, count) if given[i] < largest] or [i for i in range(1, count) if given[i] < reach]
        whole, remaining = sum([portions[i] for i in free]), rest
        for i in free:
            extra = min(reach - given[i], max(1, remaining * portions[i] // whole), rest)
            given[i] = given[i] + extra
            rest = rest - extra
    return np.array(given)


def gaussian(rng, dims, deviation, reach, shards=(), kind=jnp.bfloat16):
    gain = block_levels(rng, dims, shards, -0.22, 0.18) if shards else 1.0
    values = jax.random.normal(rng, dims, jnp.float32) * deviation * gain
    return jnp.minimum(jnp.maximum(values, -reach), reach).astype(kind)


def setup_inputs(seed: int = 0, part: int = 0) -> dict:
    key_list = jax.random.split(jax.random.key(seed), 16)
    part_keys = jax.random.split(jax.random.fold_in(key_list[15], part), 16)
    residual = gaussian(part_keys[0], (LEN, SEQS, D), 1.0, 6.0, ((0, 16),))
    query = draw_query(jax.random.fold_in(jax.random.fold_in(key_list[15], part), 71), part)
    latent = gaussian(part_keys[2], (LEN, SEQS, LATENT), 1.0, 6.0, ((0, 4),))
    rope_key = draw_rope_key(jax.random.fold_in(jax.random.fold_in(key_list[15], part), 71), part)
    latent_gain = jnp.clip(1.0 + 0.18 * jax.random.normal(key_list[4], (LATENT,), jnp.float32), 0.1, 1.9)
    key_up = gaussian(key_list[5], (LATENT, HEADS * NOPE), LATENT ** -0.5, 0.25, ((1, 4),))
    value_up = gaussian(key_list[6], (LATENT, HEADS * VDIM), LATENT ** -0.5, 0.25, ((1, 4),))
    out_weight = gaussian(key_list[7], (HEADS * VDIM, D), (HEADS * VDIM // 4) ** -0.5, 0.375, ((0, 4),))
    norm_gain = jnp.clip(1.0 + 0.18 * jax.random.normal(key_list[8], (D,), jnp.float32), 0.1, 1.9)
    group_prob = jnp.clip(jnp.exp(math.log(1.0) - 1.3862944 * jax.random.uniform(part_keys[9], (LEN, SEQS), jnp.float32) ** block_levels(part_keys[9], (LEN, SEQS), ((0, 16),), -0.2, 0.2)), 0.25, 1.0)
    pair_logits = gaussian(part_keys[10], (LEN, SEQS, TOPK), 1.5, 8.0, ((0, 16),), jnp.float32)
    routes_keys = jax.random.split(jax.random.fold_in(part_keys[11], 1), LEN * SEQS // ROWS_DEV)
    routes_turns = jax.random.permutation(jax.random.fold_in(part_keys[11], 3), LEN * SEQS // ROWS_DEV)
    routes = jax.vmap(lambda own, number: assign_block(jax.random.fold_in(part_keys[11], 2), own, number, ROWS_DEV, EXPERTS, TOPK, CAP, 1))(routes_keys, routes_turns).reshape((LEN, SEQS, TOPK))
    w_gate = gaussian(key_list[12], (EXPERTS, D, FF), D ** -0.5, 0.125, ((0, 16),))
    w_up = gaussian(key_list[13], (EXPERTS, D, FF), D ** -0.5, 0.125, ((0, 16),))
    w_down = gaussian(key_list[14], (EXPERTS, FF, D), (FF // 4) ** -0.5, 0.4375, ((0, 16),))
    return {"residual": residual, "query": query, "latent": latent, "rope_key": rope_key, "latent_gain": latent_gain, "key_up": key_up, "value_up": value_up, "out_weight": out_weight, "norm_gain": norm_gain, "group_prob": group_prob, "pair_logits": pair_logits, "routes": routes, "w_gate": w_gate, "w_up": w_up, "w_down": w_down}


epsilon = 1e-06
rotary_base = 10000.0

def rotate(values, positions):
    halfway = values.shape[-1] // 2
    inverse = rotary_base ** (-jnp.arange(halfway, dtype=jnp.float32) / halfway)
    angles = positions.astype(jnp.float32)[:, None] * inverse[None, :]
    angles = angles.reshape((angles.shape[0],) + (1,) * (values.ndim - 2) + (halfway,))
    cosine_values = jnp.cos(angles)
    sine_values = jnp.sin(angles)
    first_half = values[..., :halfway]
    second_half = values[..., halfway:]
    return jnp.concatenate([first_half * cosine_values - second_half * sine_values, second_half * cosine_values + first_half * sine_values], axis=-1)

def rms_scale(values, gain_values):
    return values * lax.rsqrt(lax.optimization_barrier(jnp.mean(values * values, axis=-1, keepdims=True)) + epsilon) * gain_values

def expand(latent_rows, latent_gain, key_up, value_up):
    normed = rms_scale(latent_rows.astype(jnp.float32), latent_gain).astype(jnp.bfloat16)
    keys_nope = jnp.dot(normed, key_up, preferred_element_type=jnp.float32).astype(jnp.bfloat16)
    values = jnp.dot(normed, value_up, preferred_element_type=jnp.float32).astype(jnp.bfloat16)
    lead = latent_rows.shape[:2]
    return (keys_nope.reshape(lead + (key_up.shape[1] // NOPE, NOPE)), values.reshape(lead + (value_up.shape[1] // VDIM, VDIM)))

def reference(residual, query, latent, rope_key, latent_gain, key_up, value_up, out_weight, norm_gain, group_prob, pair_logits, routes, w_gate, w_up, w_down):
    positions = jnp.arange(LEN, dtype=jnp.int32)
    key_nope, value_rows = expand(latent, latent_gain, key_up, value_up)
    key_rot = rotate(rope_key.astype(jnp.float32), positions).astype(jnp.bfloat16)
    split_query = query.reshape(LEN, SEQS, HEADS, QK)
    query_nope = split_query[..., :NOPE]
    query_rot = rotate(split_query[..., NOPE:].astype(jnp.float32), positions).astype(jnp.bfloat16)

    def attend(inputs):
        head_nope, head_rot, head_keys, head_values = inputs
        scores = jnp.einsum('qsd,ksd->sqk', head_nope.astype(jnp.float32), head_keys.astype(jnp.float32))
        scores = scores + jnp.einsum('qsd,ksd->sqk', head_rot.astype(jnp.float32), key_rot.astype(jnp.float32))
        scores = scores * QK ** (-0.5)
        highest = lax.optimization_barrier(jnp.max(scores, axis=-1, keepdims=True))
        weights = jnp.exp(scores - highest)
        totals = lax.optimization_barrier(jnp.sum(weights, axis=-1))
        rounded = lax.optimization_barrier(weights.astype(jnp.bfloat16)).astype(jnp.float32)
        mixed = jnp.einsum('sqk,ksd->sqd', rounded, head_values.astype(jnp.float32))
        return (mixed / totals[..., None]).astype(jnp.bfloat16)
    heads_out = lax.map(attend, (jnp.moveaxis(query_nope, 2, 0), jnp.moveaxis(query_rot, 2, 0), jnp.moveaxis(key_nope, 2, 0), jnp.moveaxis(value_rows, 2, 0)))
    row_total = LEN * SEQS
    attended = jnp.transpose(heads_out, (2, 1, 0, 3)).reshape(row_total, HEADS * VDIM)
    projected = jnp.dot(attended, out_weight, preferred_element_type=jnp.float32)
    stream = (residual.reshape(row_total, D).astype(jnp.float32) + projected).astype(jnp.bfloat16)
    normed = rms_scale(stream.astype(jnp.float32), norm_gain).astype(jnp.bfloat16)
    mixing = jax.nn.softmax(pair_logits.reshape(row_total, TOPK), axis=-1) * group_prob.reshape(row_total, 1)
    blocks = row_total // ROWS_DEV
    chosen = routes.reshape(blocks, ROWS_DEV * TOPK).astype(jnp.int32)
    one_hot = (chosen[..., None] == jnp.arange(EXPERTS, dtype=jnp.int32)).astype(jnp.int32)
    before = jnp.cumsum(one_hot, axis=1) - one_hot
    slot_index = lax.optimization_barrier(jnp.sum(before * one_hot, axis=-1)).astype(jnp.int32)
    column = (jnp.arange(blocks, dtype=jnp.int32)[:, None] * CAP + slot_index).astype(jnp.int32)
    source_row = (jnp.arange(row_total * TOPK, dtype=jnp.int32).reshape(blocks, ROWS_DEV * TOPK) // TOPK).astype(jnp.int32)
    slot_table = jnp.full((EXPERTS, blocks * CAP), row_total, jnp.int32).at[chosen, column].set(source_row)
    padded = jnp.concatenate([normed, jnp.zeros((1, D), jnp.bfloat16)], axis=0)

    def serve_rows(expert_inputs):
        row_numbers, gate_weight, up_weight, down_weight = expert_inputs
        gathered = padded[row_numbers]
        gate_pre = jnp.dot(gathered, gate_weight, preferred_element_type=jnp.float32)
        upward = jnp.dot(gathered, up_weight, preferred_element_type=jnp.float32)
        hidden = (jax.nn.silu(gate_pre) * upward).astype(jnp.bfloat16)
        return jnp.dot(hidden, down_weight, preferred_element_type=jnp.float32).astype(jnp.bfloat16)
    served = lax.map(serve_rows, (slot_table, w_gate, w_up, w_down))
    results = served[chosen, column].reshape(row_total, TOPK, D)
    combined = stream.astype(jnp.float32) + lax.optimization_barrier(jnp.sum(results.astype(jnp.float32) * mixing[..., None], axis=1))
    return combined.astype(jnp.bfloat16).reshape(LEN, SEQS, D)
```

```python
import jax
import jax.numpy as jnp
from jax import lax
from jax.sharding import PartitionSpec as P

D = 2048
NOPE = 128
VDIM = 128
QK = 192
TOPK = 2
SEQS = 4


epsilon = 1e-06
rotary_base = 10000.0
lowest = -1e30


def rotate(values, positions):
    halfway = values.shape[-1] // 2
    inverse = rotary_base ** (-jnp.arange(halfway, dtype=jnp.float32) / halfway)
    angles = positions.astype(jnp.float32)[:, None] * inverse[None, :]
    angles = angles.reshape((angles.shape[0],) + (1,) * (values.ndim - 2) + (halfway,))
    cosine_values = jnp.cos(angles)
    sine_values = jnp.sin(angles)
    first_half = values[..., :halfway]
    second_half = values[..., halfway:]
    return jnp.concatenate(
        [
            first_half * cosine_values - second_half * sine_values,
            second_half * cosine_values + first_half * sine_values,
        ],
        axis=-1,
    )


def rms_scale(values, gain_values):
    return (
        values
        * lax.rsqrt(jnp.mean(values * values, axis=-1, keepdims=True) + epsilon)
        * gain_values
    )


def expand(latent_rows, latent_gain, key_up, value_up):
    normed = rms_scale(latent_rows.astype(jnp.float32), latent_gain).astype(jnp.bfloat16)
    keys_nope = jnp.dot(normed, key_up, preferred_element_type=jnp.float32).astype(jnp.bfloat16)
    values = jnp.dot(normed, value_up, preferred_element_type=jnp.float32).astype(jnp.bfloat16)
    lead = latent_rows.shape[:2]
    return (
        keys_nope.reshape(lead + (key_up.shape[1] // NOPE, NOPE)),
        values.reshape(lead + (value_up.shape[1] // VDIM, VDIM)),
    )


def absorb(carried, query_nope, query_rot, key_nope, value_rows, key_rot):
    running, totals, accumulated = carried
    scores = jnp.einsum("qshd,kshd->qshk", query_nope, key_nope, preferred_element_type=jnp.float32)
    scores = scores + jnp.einsum(
        "qshd,ksd->qshk", query_rot, key_rot, preferred_element_type=jnp.float32
    )
    scores = scores * QK ** (-0.5)
    highest = jnp.maximum(running, jnp.max(scores, axis=-1))
    weights = jnp.exp(scores - highest[..., None])
    totals = jnp.sum(weights, axis=-1)
    accumulated = jnp.einsum(
        "qshk,kshd->qshd",
        weights.astype(jnp.bfloat16),
        value_rows,
        preferred_element_type=jnp.float32,
    )
    return (highest, totals, accumulated)


def slots(chosen, row_count, experts_total):
    capacity = max(2, 3 * row_count * TOPK // (2 * experts_total))
    capacity = -(-capacity // 8) * 8
    one_hot = (chosen[:, None] == jnp.arange(experts_total, dtype=jnp.int32)[None, :]).astype(
        jnp.bfloat16
    )
    order = jnp.arange(chosen.shape[0])
    earlier = (order[:, None] > order[None, :]).astype(jnp.bfloat16)
    before = jnp.dot(earlier, one_hot, preferred_element_type=jnp.float32)
    slot_index = jnp.sum(before * one_hot.astype(jnp.float32), axis=-1).astype(jnp.int32)
    return capacity, chosen * capacity + slot_index


def whole_out_weight(out_weight):
    pieces = lax.axis_size("sp")
    depth = out_weight.shape[0] // pieces
    own = lax.dynamic_slice_in_dim(out_weight, lax.axis_index("sp") * depth, depth, axis=0)
    return lax.all_gather(own, ("tp", "sp"), axis=0, tiled=True)


def shards(
    residual,
    query,
    latent,
    rope_key,
    latent_gain,
    key_up,
    value_up,
    out_weight,
    norm_gain,
    group_prob,
    pair_logits,
    routes,
    w_gate,
    w_up,
    w_down,
):
    positions_here = query.shape[0]
    heads_here = key_up.shape[1] // NOPE
    own_positions = lax.axis_index("sp") * positions_here + jnp.arange(
        positions_here, dtype=jnp.int32
    )
    split_query = query.reshape(positions_here, SEQS, heads_here, QK)
    query_nope = split_query[..., :NOPE]
    query_rot = rotate(split_query[..., NOPE:].astype(jnp.float32), own_positions).astype(
        jnp.bfloat16
    )
    key_rot = rotate(rope_key.astype(jnp.float32), own_positions).astype(jnp.bfloat16)
    initial = (
        jnp.full((positions_here, SEQS, heads_here), lowest, jnp.float32),
        jnp.zeros((positions_here, SEQS, heads_here), jnp.float32),
        jnp.zeros((positions_here, SEQS, heads_here, VDIM), jnp.float32),
    )
    key_nope, value_rows = expand(
        lax.all_gather(latent, "sp", axis=0, tiled=True), latent_gain, key_up, value_up
    )
    finished = absorb(
        initial,
        query_nope,
        query_rot,
        key_nope,
        value_rows,
        lax.all_gather(key_rot, "sp", axis=0, tiled=True),
    )
    attended = (finished[2] / finished[1][..., None]).astype(jnp.bfloat16)
    attended = attended.reshape(positions_here, SEQS, heads_here * VDIM)
    by_token = lax.all_to_all(attended, "tp", split_axis=0, concat_axis=2, tiled=True)
    row_count = by_token.shape[0] * SEQS
    mixed_heads = by_token.reshape(row_count, by_token.shape[2])
    projected = jnp.dot(
        mixed_heads,
        whole_out_weight(out_weight),
        preferred_element_type=jnp.float32,
    )
    stream = (residual.reshape(row_count, D).astype(jnp.float32) + projected).astype(jnp.bfloat16)
    normed = rms_scale(stream.astype(jnp.float32), norm_gain).astype(jnp.bfloat16)
    mixing = jax.nn.softmax(pair_logits.reshape(row_count, TOPK), axis=-1) * group_prob.reshape(
        row_count, 1
    )
    experts_total = lax.axis_size("sp") * lax.axis_size("tp")
    capacity, target = slots(routes.reshape(row_count * TOPK), row_count, experts_total)
    spots = target.reshape(row_count, TOPK)
    places = jnp.arange(experts_total * capacity, dtype=jnp.int32)
    picked = spots[:, :, None] == places[None, None, :]
    pick_rows = jnp.any(picked, axis=1).astype(jnp.bfloat16)
    outgoing = lax.dot_general(
        pick_rows, normed, (((0,), (0,)), ((), ())), preferred_element_type=jnp.float32
    ).astype(jnp.bfloat16)
    outgoing = outgoing.reshape(experts_total, capacity, D)
    arrived = lax.all_to_all(outgoing, ("sp", "tp"), split_axis=0, concat_axis=0, tiled=True)
    flat_rows = arrived.reshape(-1, D)
    gate_pre = jnp.dot(flat_rows, w_gate[0], preferred_element_type=jnp.float32)
    upward = jnp.dot(flat_rows, w_up[0], preferred_element_type=jnp.float32)
    hidden = (jax.nn.silu(gate_pre) * upward).astype(jnp.bfloat16)
    served = (
        jnp.dot(hidden, w_down[0], preferred_element_type=jnp.float32)
        .astype(jnp.bfloat16)
        .reshape(arrived.shape)
    )
    returned = lax.all_to_all(served, ("sp", "tp"), split_axis=0, concat_axis=0, tiled=True)
    returned = returned.reshape(experts_total * capacity, D)
    combined = stream.astype(jnp.float32)
    for choice in range(TOPK):
        combined = combined + mixing[:, choice, None] * jnp.dot(
            picked[:, choice].astype(jnp.bfloat16), returned, preferred_element_type=jnp.float32
        )
    return combined.astype(jnp.bfloat16).reshape(residual.shape)


def solution(mesh):
    placed = (
        P(("sp", "tp"), "grp", None),
        P("sp", "grp", "tp"),
        P("sp", "grp", None),
        P("sp", "grp", None),
        P(),
        P(None, "tp"),
        P(None, "tp"),
        P("tp", None),
        P(),
        P(("sp", "tp"), "grp"),
        P(("sp", "tp"), "grp", None),
        P(("sp", "tp"), "grp", None),
        P(("sp", "tp"), None, None),
        P(("sp", "tp"), None, None),
        P(("sp", "tp"), None, None),
    )
    return jax.shard_map(
        shards, mesh=mesh, in_specs=placed, out_specs=P(("sp", "tp"), "grp", None), check_vma=False
    )
```

```python
import jax
import jax.numpy as jnp
from jax import lax
from jax.experimental import pallas as pl
from jax.experimental.pallas import tpu as pltpu
from jax.sharding import PartitionSpec as P

D = 2048
NOPE = 128
VDIM = 128
QK = 192
TOPK = 2
SEQS = 4


epsilon = 1e-06
rotary_base = 10000.0
lowest = -1e30


def rotate(values, positions):
    halfway = values.shape[-1] // 2
    inverse = rotary_base ** (-jnp.arange(halfway, dtype=jnp.float32) / halfway)
    angles = positions.astype(jnp.float32)[:, None] * inverse[None, :]
    angles = angles.reshape((angles.shape[0],) + (1,) * (values.ndim - 2) + (halfway,))
    cosine_values = jnp.cos(angles)
    sine_values = jnp.sin(angles)
    first_half = values[..., :halfway]
    second_half = values[..., halfway:]
    return jnp.concatenate(
        [
            first_half * cosine_values - second_half * sine_values,
            second_half * cosine_values + first_half * sine_values,
        ],
        axis=-1,
    )


def rms_scale(values, gain_values):
    return (
        values
        * lax.rsqrt(jnp.mean(values * values, axis=-1, keepdims=True) + epsilon)
        * gain_values
    )


def expand(latent_rows, latent_gain, key_up, value_up):
    normed = rms_scale(latent_rows.astype(jnp.float32), latent_gain).astype(jnp.bfloat16)
    keys_nope = jnp.dot(normed, key_up, preferred_element_type=jnp.float32).astype(jnp.bfloat16)
    values = jnp.dot(normed, value_up, preferred_element_type=jnp.float32).astype(jnp.bfloat16)
    lead = latent_rows.shape[:2]
    return (
        keys_nope.reshape(lead + (key_up.shape[1] // NOPE, NOPE)),
        values.reshape(lead + (value_up.shape[1] // VDIM, VDIM)),
    )


def absorb(carried, query_nope, query_rot, key_nope, value_rows, key_rot):
    running, totals, accumulated = carried
    scores = jnp.einsum("qshd,kshd->qshk", query_nope, key_nope, preferred_element_type=jnp.float32)
    scores = scores + jnp.einsum(
        "qshd,ksd->qshk", query_rot, key_rot, preferred_element_type=jnp.float32
    )
    scores = scores * QK ** (-0.5)
    highest = jnp.maximum(running, jnp.max(scores, axis=-1))
    weights = jnp.exp(scores - highest[..., None])
    totals = jnp.sum(weights, axis=-1)
    accumulated = jnp.einsum(
        "qshk,kshd->qshd",
        weights.astype(jnp.bfloat16),
        value_rows,
        preferred_element_type=jnp.float32,
    )
    return (highest, totals, accumulated)


def slots(chosen, row_count, experts_total):
    capacity = max(2, 3 * row_count * TOPK // (2 * experts_total))
    capacity = -(-capacity // 8) * 8
    one_hot = (chosen[:, None] == jnp.arange(experts_total, dtype=jnp.int32)[None, :]).astype(
        jnp.bfloat16
    )
    order = jnp.arange(chosen.shape[0])
    earlier = (order[:, None] > order[None, :]).astype(jnp.bfloat16)
    before = jnp.dot(earlier, one_hot, preferred_element_type=jnp.float32)
    slot_index = jnp.sum(before * one_hot.astype(jnp.float32), axis=-1).astype(jnp.int32)
    return capacity, chosen * capacity + slot_index


def whole_out_weight(out_weight):
    copies = ("grp", "sp")
    depth = out_weight.shape[0] // lax.axis_size(copies)
    own = lax.dynamic_slice_in_dim(out_weight, lax.axis_index(copies) * depth, depth, axis=0)
    return lax.all_gather(own, ("tp",) + copies, axis=0, tiled=True)


def gather_kernel(chips, pieces, latent_ref, rot_ref, latent_out, rot_out, *sems):
    near_send, near_recv, far_send, far_recv, own_sem = sems
    me = lax.axis_index("sp")
    chip, core = me // 2, lax.rem(me, 2)
    mate = chip * 2 + 1 - core
    mesh_id = pl.DeviceIdType.MESH

    def peer(step):
        return lax.rem(chip + step, chips) * 2 + core

    barrier = pltpu.get_barrier_semaphore()
    pl.semaphore_signal(barrier, inc=1, device_id={"sp": mate}, device_id_type=mesh_id)
    for step in range(1, chips):
        pl.semaphore_signal(barrier, inc=1, device_id={"sp": peer(step)}, device_id_type=mesh_id)
    pl.semaphore_wait(barrier, chips)

    rows = latent_ref.shape[0] // pieces

    def views(slot, piece, own):
        if piece == pieces:
            return (rot_ref if own else rot_out.at[slot]), rot_out.at[slot]
        part = pl.ds(piece * rows, rows)
        target = latent_out.at[slot, part]
        return (latent_ref.at[part] if own else target), target

    def remote(slot, piece, own, send, recv, device):
        source, target = views(slot, piece, own)
        copy = pltpu.make_async_remote_copy(
            src_ref=source,
            dst_ref=target,
            send_sem=send,
            recv_sem=recv,
            device_id={"sp": device},
            device_id_type=mesh_id,
        )
        copy.start()
        return copy

    order = [pieces] + list(range(pieces))
    far = {}
    for step in range(1, chips):
        for piece in order:
            far[step, piece] = remote(
                me, piece, True, far_send.at[step, piece], far_recv.at[step, piece], peer(step)
            )
    near = []
    for piece in order:
        near.append(
            remote(me, piece, True, near_send.at[0, piece], near_recv.at[0, piece], mate)
        )
    kept = [
        pltpu.make_async_copy(latent_ref, latent_out.at[me], own_sem.at[0]),
        pltpu.make_async_copy(rot_ref, rot_out.at[me], own_sem.at[1]),
    ]
    for copy in kept:
        copy.start()
    for step in range(1, chips):
        slot = peer(chips - step)
        for piece in order:
            far[step, piece].wait_recv()
            near.append(
                remote(
                    slot, piece, False, near_send.at[step, piece], near_recv.at[step, piece], mate
                )
            )
    for copy in kept:
        copy.wait()
    for copy in far.values():
        copy.wait_send()
    for copy in near:
        copy.wait()


def gather_keys(latent, key_rot):
    count = lax.axis_size("sp")
    chips, pieces = count // 2, 6
    outs = pl.pallas_call(
        lambda *refs: gather_kernel(chips, pieces, *refs),
        out_shape=[
            jax.ShapeDtypeStruct((count,) + latent.shape, latent.dtype),
            jax.ShapeDtypeStruct((count,) + key_rot.shape, key_rot.dtype),
        ],
        in_specs=[pl.BlockSpec(memory_space=pl.ANY)] * 2,
        out_specs=[pl.BlockSpec(memory_space=pl.ANY)] * 2,
        scratch_shapes=[pltpu.SemaphoreType.DMA((chips, pieces + 1))] * 4
        + [pltpu.SemaphoreType.DMA((2,))],
        compiler_params=pltpu.CompilerParams(collective_id=0, has_side_effects=True),
        name="gather_keys",
    )(latent, key_rot)
    return [whole.reshape((-1,) + whole.shape[2:]) for whole in outs]


def shards(
    residual,
    query,
    latent,
    rope_key,
    latent_gain,
    key_up,
    value_up,
    out_weight,
    norm_gain,
    group_prob,
    pair_logits,
    routes,
    w_gate,
    w_up,
    w_down,
):
    positions_here = query.shape[0]
    heads_here = key_up.shape[1] // NOPE
    own_positions = lax.axis_index("sp") * positions_here + jnp.arange(
        positions_here, dtype=jnp.int32
    )
    split_query = query.reshape(positions_here, SEQS, heads_here, QK)
    query_nope = split_query[..., :NOPE]
    query_rot = rotate(split_query[..., NOPE:].astype(jnp.float32), own_positions).astype(
        jnp.bfloat16
    )
    key_rot = rotate(rope_key.astype(jnp.float32), own_positions).astype(jnp.bfloat16)
    initial = (
        jnp.full((positions_here, SEQS, heads_here), lowest, jnp.float32),
        jnp.zeros((positions_here, SEQS, heads_here), jnp.float32),
        jnp.zeros((positions_here, SEQS, heads_here, VDIM), jnp.float32),
    )
    all_latent, all_key_rot = gather_keys(latent, key_rot)
    key_nope, value_rows = expand(all_latent, latent_gain, key_up, value_up)
    finished = absorb(
        initial,
        query_nope,
        query_rot,
        key_nope,
        value_rows,
        all_key_rot,
    )
    attended = (finished[2] / finished[1][..., None]).astype(jnp.bfloat16)
    attended = attended.reshape(positions_here, SEQS, heads_here * VDIM)
    by_token = lax.all_to_all(attended, "tp", split_axis=0, concat_axis=2, tiled=True)
    row_count = by_token.shape[0] * SEQS
    mixed_heads = by_token.reshape(row_count, by_token.shape[2])
    projected = jnp.dot(
        mixed_heads,
        whole_out_weight(out_weight),
        preferred_element_type=jnp.float32,
    )
    stream = (residual.reshape(row_count, D).astype(jnp.float32) + projected).astype(jnp.bfloat16)
    normed = rms_scale(stream.astype(jnp.float32), norm_gain).astype(jnp.bfloat16)
    mixing = jax.nn.softmax(pair_logits.reshape(row_count, TOPK), axis=-1) * group_prob.reshape(
        row_count, 1
    )
    experts_total = lax.axis_size("sp") * lax.axis_size("tp")
    capacity, target = slots(routes.reshape(row_count * TOPK), row_count, experts_total)
    spots = target.reshape(row_count, TOPK)
    places = jnp.arange(experts_total * capacity, dtype=jnp.int32)
    picked = spots[:, :, None] == places[None, None, :]
    pick_rows = jnp.any(picked, axis=1).astype(jnp.bfloat16)
    outgoing = lax.dot_general(
        pick_rows, normed, (((0,), (0,)), ((), ())), preferred_element_type=jnp.float32
    ).astype(jnp.bfloat16)
    outgoing = outgoing.reshape(experts_total, capacity, D)
    arrived = lax.all_to_all(outgoing, ("sp", "tp"), split_axis=0, concat_axis=0, tiled=True)
    flat_rows = arrived.reshape(-1, D)
    gate_pre = jnp.dot(flat_rows, w_gate[0], preferred_element_type=jnp.float32)
    upward = jnp.dot(flat_rows, w_up[0], preferred_element_type=jnp.float32)
    hidden = (jax.nn.silu(gate_pre) * upward).astype(jnp.bfloat16)
    served = (
        jnp.dot(hidden, w_down[0], preferred_element_type=jnp.float32)
        .astype(jnp.bfloat16)
        .reshape(arrived.shape)
    )
    returned = lax.all_to_all(served, ("sp", "tp"), split_axis=0, concat_axis=0, tiled=True)
    returned = returned.reshape(experts_total * capacity, D)
    combined = stream.astype(jnp.float32)
    for choice in range(TOPK):
        combined = combined + mixing[:, choice, None] * jnp.dot(
            picked[:, choice].astype(jnp.bfloat16), returned, preferred_element_type=jnp.float32
        )
    return combined.astype(jnp.bfloat16).reshape(residual.shape)


def solution(mesh):
    placed = (
        P(("sp", "tp"), "grp", None),
        P("sp", "grp", "tp"),
        P("sp", "grp", None),
        P("sp", "grp", None),
        P(),
        P(None, "tp"),
        P(None, "tp"),
        P("tp", None),
        P(),
        P(("sp", "tp"), "grp"),
        P(("sp", "tp"), "grp", None),
        P(("sp", "tp"), "grp", None),
        P(("sp", "tp"), None, None),
        P(("sp", "tp"), None, None),
        P(("sp", "tp"), None, None),
    )
    return jax.shard_map(
        shards, mesh=mesh, in_specs=placed, out_specs=P(("sp", "tp"), "grp", None), check_vma=False
    )
```

```python
import jax
import jax.numpy as jnp
from jax import lax
from jax.experimental import pallas as pl
from jax.experimental.pallas import tpu as pltpu
from jax.sharding import PartitionSpec as P

D = 2048
NOPE = 128
VDIM = 128
QK = 192
TOPK = 2
SEQS = 4


epsilon = 1e-06
rotary_base = 10000.0
lowest = -1e30


def rotate(values, positions):
    halfway = values.shape[-1] // 2
    inverse = rotary_base ** (-jnp.arange(halfway, dtype=jnp.float32) / halfway)
    angles = positions.astype(jnp.float32)[:, None] * inverse[None, :]
    angles = angles.reshape((angles.shape[0],) + (1,) * (values.ndim - 2) + (halfway,))
    cosine_values = jnp.cos(angles)
    sine_values = jnp.sin(angles)
    first_half = values[..., :halfway]
    second_half = values[..., halfway:]
    return jnp.concatenate(
        [
            first_half * cosine_values - second_half * sine_values,
            second_half * cosine_values + first_half * sine_values,
        ],
        axis=-1,
    )


def rms_scale(values, gain_values):
    return (
        values
        * lax.rsqrt(jnp.mean(values * values, axis=-1, keepdims=True) + epsilon)
        * gain_values
    )


def expand(latent_rows, latent_gain, key_up, value_up):
    normed = rms_scale(latent_rows.astype(jnp.float32), latent_gain).astype(jnp.bfloat16)
    keys_nope = jnp.dot(normed, key_up, preferred_element_type=jnp.float32).astype(jnp.bfloat16)
    values = jnp.dot(normed, value_up, preferred_element_type=jnp.float32).astype(jnp.bfloat16)
    lead = latent_rows.shape[:2]
    return (
        keys_nope.reshape(lead + (key_up.shape[1] // NOPE, NOPE)),
        values.reshape(lead + (value_up.shape[1] // VDIM, VDIM)),
    )


def absorb(carried, query_nope, query_rot, key_nope, value_rows, key_rot):
    running, totals, accumulated = carried
    scores = jnp.einsum("qshd,kshd->qshk", query_nope, key_nope, preferred_element_type=jnp.float32)
    scores = scores + jnp.einsum(
        "qshd,ksd->qshk", query_rot, key_rot, preferred_element_type=jnp.float32
    )
    scores = scores * QK ** (-0.5)
    highest = jnp.maximum(running, jnp.max(scores, axis=-1))
    weights = jnp.exp(scores - highest[..., None])
    totals = jnp.sum(weights, axis=-1)
    accumulated = jnp.einsum(
        "qshk,kshd->qshd",
        weights.astype(jnp.bfloat16),
        value_rows,
        preferred_element_type=jnp.float32,
    )
    return (highest, totals, accumulated)


def slots(chosen, row_count, experts_total):
    capacity = max(2, 3 * row_count * TOPK // (2 * experts_total))
    capacity = -(-capacity // 8) * 8
    one_hot = (chosen[:, None] == jnp.arange(experts_total, dtype=jnp.int32)[None, :]).astype(
        jnp.bfloat16
    )
    order = jnp.arange(chosen.shape[0])
    earlier = (order[:, None] > order[None, :]).astype(jnp.bfloat16)
    before = jnp.dot(earlier, one_hot, preferred_element_type=jnp.float32)
    slot_index = jnp.sum(before * one_hot.astype(jnp.float32), axis=-1).astype(jnp.int32)
    return capacity, chosen * capacity + slot_index


def whole_out_weight(out_weight, after):
    copies = ("grp", "sp")
    depth = out_weight.shape[0] // lax.axis_size(copies)
    own = lax.dynamic_slice_in_dim(out_weight, lax.axis_index(copies) * depth, depth, axis=0)
    own, after = lax.optimization_barrier((own, after))
    return after, lax.all_gather(own, ("tp",) + copies, axis=0, tiled=True)


def gather_kernel(chips, pieces, latent_ref, rot_ref, latent_out, rot_out, *sems):
    near_send, near_recv, far_send, far_recv, own_sem = sems
    me = lax.axis_index("sp")
    chip, core = me // 2, lax.rem(me, 2)
    mate = chip * 2 + 1 - core
    mesh_id = pl.DeviceIdType.MESH

    def peer(step):
        return lax.rem(chip + step, chips) * 2 + core

    barrier = pltpu.get_barrier_semaphore()
    pl.semaphore_signal(barrier, inc=1, device_id={"sp": mate}, device_id_type=mesh_id)
    for step in range(1, chips):
        pl.semaphore_signal(barrier, inc=1, device_id={"sp": peer(step)}, device_id_type=mesh_id)
    pl.semaphore_wait(barrier, chips)

    rows = latent_ref.shape[0] // pieces

    def views(slot, piece, own):
        if piece == pieces:
            return (rot_ref if own else rot_out.at[slot]), rot_out.at[slot]
        part = pl.ds(piece * rows, rows)
        target = latent_out.at[slot, part]
        return (latent_ref.at[part] if own else target), target

    def remote(slot, piece, own, send, recv, device):
        source, target = views(slot, piece, own)
        copy = pltpu.make_async_remote_copy(
            src_ref=source,
            dst_ref=target,
            send_sem=send,
            recv_sem=recv,
            device_id={"sp": device},
            device_id_type=mesh_id,
        )
        copy.start()
        return copy

    order = [pieces] + list(range(pieces))
    far = {}
    for step in range(1, chips):
        for piece in order:
            far[step, piece] = remote(
                me, piece, True, far_send.at[step, piece], far_recv.at[step, piece], peer(step)
            )
    near = []
    for piece in order:
        near.append(
            remote(me, piece, True, near_send.at[0, piece], near_recv.at[0, piece], mate)
        )
    kept = [
        pltpu.make_async_copy(latent_ref, latent_out.at[me], own_sem.at[0]),
        pltpu.make_async_copy(rot_ref, rot_out.at[me], own_sem.at[1]),
    ]
    for copy in kept:
        copy.start()
    for step in range(1, chips):
        slot = peer(chips - step)
        for piece in order:
            far[step, piece].wait_recv()
            near.append(
                remote(
                    slot, piece, False, near_send.at[step, piece], near_recv.at[step, piece], mate
                )
            )
    for copy in kept:
        copy.wait()
    for copy in far.values():
        copy.wait_send()
    for copy in near:
        copy.wait()


def gather_keys(latent, key_rot):
    count = lax.axis_size("sp")
    chips, pieces = count // 2, 6
    outs = pl.pallas_call(
        lambda *refs: gather_kernel(chips, pieces, *refs),
        out_shape=[
            jax.ShapeDtypeStruct((count,) + latent.shape, latent.dtype),
            jax.ShapeDtypeStruct((count,) + key_rot.shape, key_rot.dtype),
        ],
        in_specs=[pl.BlockSpec(memory_space=pl.ANY)] * 2,
        out_specs=[pl.BlockSpec(memory_space=pl.ANY)] * 2,
        scratch_shapes=[pltpu.SemaphoreType.DMA((chips, pieces + 1))] * 4
        + [pltpu.SemaphoreType.DMA((2,))],
        compiler_params=pltpu.CompilerParams(collective_id=0, has_side_effects=True),
        name="gather_keys",
    )(latent, key_rot)
    return [whole.reshape((-1,) + whole.shape[2:]) for whole in outs]


def shards(
    residual,
    query,
    latent,
    rope_key,
    latent_gain,
    key_up,
    value_up,
    out_weight,
    norm_gain,
    group_prob,
    pair_logits,
    routes,
    w_gate,
    w_up,
    w_down,
):
    positions_here = query.shape[0]
    heads_here = key_up.shape[1] // NOPE
    own_positions = lax.axis_index("sp") * positions_here + jnp.arange(
        positions_here, dtype=jnp.int32
    )
    split_query = query.reshape(positions_here, SEQS, heads_here, QK)
    query_nope = split_query[..., :NOPE]
    query_rot = rotate(split_query[..., NOPE:].astype(jnp.float32), own_positions).astype(
        jnp.bfloat16
    )
    key_rot = rotate(rope_key.astype(jnp.float32), own_positions).astype(jnp.bfloat16)
    initial = (
        jnp.full((positions_here, SEQS, heads_here), lowest, jnp.float32),
        jnp.zeros((positions_here, SEQS, heads_here), jnp.float32),
        jnp.zeros((positions_here, SEQS, heads_here, VDIM), jnp.float32),
    )
    all_latent, all_key_rot = gather_keys(latent, key_rot)
    all_key_rot, gathered_weight = whole_out_weight(out_weight, all_key_rot)
    key_nope, value_rows = expand(all_latent, latent_gain, key_up, value_up)
    finished = absorb(
        initial,
        query_nope,
        query_rot,
        key_nope,
        value_rows,
        all_key_rot,
    )
    attended = (finished[2] / finished[1][..., None]).astype(jnp.bfloat16)
    attended = attended.reshape(positions_here, SEQS, heads_here * VDIM)
    by_token = lax.all_to_all(attended, "tp", split_axis=0, concat_axis=2, tiled=True)
    row_count = by_token.shape[0] * SEQS
    mixed_heads = by_token.reshape(row_count, by_token.shape[2])
    projected = jnp.dot(
        mixed_heads,
        gathered_weight,
        preferred_element_type=jnp.float32,
    )
    stream = (residual.reshape(row_count, D).astype(jnp.float32) + projected).astype(jnp.bfloat16)
    normed = rms_scale(stream.astype(jnp.float32), norm_gain).astype(jnp.bfloat16)
    mixing = jax.nn.softmax(pair_logits.reshape(row_count, TOPK), axis=-1) * group_prob.reshape(
        row_count, 1
    )
    experts_total = lax.axis_size("sp") * lax.axis_size("tp")
    capacity, target = slots(routes.reshape(row_count * TOPK), row_count, experts_total)
    spots = target.reshape(row_count, TOPK)
    places = jnp.arange(experts_total * capacity, dtype=jnp.int32)
    picked = spots[:, :, None] == places[None, None, :]
    pick_rows = jnp.any(picked, axis=1).astype(jnp.bfloat16)
    outgoing = lax.dot_general(
        pick_rows, normed, (((0,), (0,)), ((), ())), preferred_element_type=jnp.float32
    ).astype(jnp.bfloat16)
    outgoing = outgoing.reshape(experts_total, capacity, D)
    arrived = lax.all_to_all(outgoing, ("sp", "tp"), split_axis=0, concat_axis=0, tiled=True)
    flat_rows = arrived.reshape(-1, D)
    gate_pre = jnp.dot(flat_rows, w_gate[0], preferred_element_type=jnp.float32)
    upward = jnp.dot(flat_rows, w_up[0], preferred_element_type=jnp.float32)
    hidden = (jax.nn.silu(gate_pre) * upward).astype(jnp.bfloat16)
    served = (
        jnp.dot(hidden, w_down[0], preferred_element_type=jnp.float32)
        .astype(jnp.bfloat16)
        .reshape(arrived.shape)
    )
    returned = lax.all_to_all(served, ("sp", "tp"), split_axis=0, concat_axis=0, tiled=True)
    returned = returned.reshape(experts_total * capacity, D)
    combined = stream.astype(jnp.float32)
    for choice in range(TOPK):
        combined = combined + mixing[:, choice, None] * jnp.dot(
            picked[:, choice].astype(jnp.bfloat16), returned, preferred_element_type=jnp.float32
        )
    return combined.astype(jnp.bfloat16).reshape(residual.shape)


def solution(mesh):
    placed = (
        P(("sp", "tp"), "grp", None),
        P("sp", "grp", "tp"),
        P("sp", "grp", None),
        P("sp", "grp", None),
        P(),
        P(None, "tp"),
        P(None, "tp"),
        P("tp", None),
        P(),
        P(("sp", "tp"), "grp"),
        P(("sp", "tp"), "grp", None),
        P(("sp", "tp"), "grp", None),
        P(("sp", "tp"), None, None),
        P(("sp", "tp"), None, None),
        P(("sp", "tp"), None, None),
    )
    return jax.shard_map(
        shards, mesh=mesh, in_specs=placed, out_specs=P(("sp", "tp"), "grp", None), check_vma=False
    )
```
